32 devices in a mesh: sp: 4 (over y, core), dp: 8 (over z, x).
Axes of the slice: x: 2, y: 2, z: 4, core: 2. Of those that a mesh axis runs over, the one named last changes fastest.
Arguments:
- queries: bfloat16 [8, 1024, 1024], P('dp', 'sp'), may hold values from -250 to 250
- keys: bfloat16 [8, 1024, 1024], P('dp', 'sp'), may hold values from -6 to 6
- values: bfloat16 [8, 1024, 1024], P('dp', 'sp'), may hold values from -6 to 6
- cum_gate: float32 [8, 16, 1024], P('dp', 'sp'), may hold values from -1024 to 0, as said below
- out_weight: bfloat16 [1024, 2112], P(None, 'dp'), may hold values from -1.5 to 1.5
Outputs:
- mixed: bfloat16 [8, 1024, 2112], P('dp', 'sp')
The draws below stay inside these ranges and needn't reach their ends.
Inputs may be any that keep to these rules, and one draw needn't show every extreme that they name: `cum_gate`: within each head the entries do not rise along positions.
All inputs are finite; a program needn't handle non-finite values.
Results may differ from the reference program's by a relative error of at most 0.0053.
Values may be sent and summed in bfloat16 or wider, within the bound.
A program may use at most 64 MiB of HBM per device.

```python
import jax
import jax.numpy as jnp
from jax import lax

D = 2112
HEAD_COUNT = 16
HEAD_DIM = 64
TOK_DEV = 256
WIDTH = 1024
SEQUENCE_LENGTH = 1024
SEQUENCE_COUNT = 8


def drawn_pair(key):
    key_query, key_key = jax.random.split(jax.random.fold_in(key, 11), 2)
    query_draw = 1.5 * jnp.clip(jax.random.normal(key_query, (SEQUENCE_COUNT, SEQUENCE_LENGTH, WIDTH), jnp.float32), -6.0, 6.0)
    key_draw = jnp.clip(jax.random.normal(key_key, (SEQUENCE_COUNT, SEQUENCE_LENGTH, WIDTH), jnp.float32), -6.0, 6.0)
    return (query_draw, key_draw)


def draw_queries(key, part):
    return drawn_pair(key)[0].astype(jnp.bfloat16)


def draw_keys(key, part):
    return drawn_pair(key)[1].astype(jnp.bfloat16)


def draw_values(key, part):
    base = jax.random.normal(jax.random.fold_in(key, 31), (SEQUENCE_COUNT, SEQUENCE_LENGTH, WIDTH), jnp.float32)
    return jnp.clip(base, -6.0, 6.0).astype(jnp.bfloat16)


def draw_cum_gate(key, part):
    key_heads, key_slow, key_fast, key_block, key_rough, key_place, key_loss = jax.random.split(jax.random.fold_in(key, 23), 7)
    head_order = jax.random.permutation(key_heads, HEAD_COUNT)
    sluggish_head = head_order < HEAD_COUNT // 2
    sluggish_head = sluggish_head[None, :, None]
    slow_rate = jax.random.uniform(key_slow, (SEQUENCE_COUNT, HEAD_COUNT, 1), jnp.float32, 0.3, 1.0) / SEQUENCE_LENGTH
    fast_rate = jax.random.uniform(key_fast, (SEQUENCE_COUNT, HEAD_COUNT, 1), jnp.float32, 1.0 / 100.0, 1.0 / 30.0)
    baseline_decay = jnp.where(sluggish_head, slow_rate, fast_rate)
    shard_count = SEQUENCE_LENGTH // TOK_DEV
    block_multiplier = jnp.exp(jax.random.uniform(key_block, (SEQUENCE_COUNT, HEAD_COUNT, shard_count, 1), jnp.float32, jnp.log(0.5), jnp.log(2.0)))
    block_multiplier = jnp.broadcast_to(block_multiplier, (SEQUENCE_COUNT, HEAD_COUNT, shard_count, TOK_DEV)).reshape(SEQUENCE_COUNT, HEAD_COUNT, SEQUENCE_LENGTH)
    jitter_level = jax.random.uniform(key_rough, (SEQUENCE_COUNT, HEAD_COUNT, SEQUENCE_LENGTH), jnp.float32, 0.3, 1.7)
    spike_locations = jax.random.randint(key_place, (SEQUENCE_COUNT, HEAD_COUNT, 3), 0, SEQUENCE_LENGTH)
    decay_amounts = jax.random.uniform(key_loss, (SEQUENCE_COUNT, HEAD_COUNT, 3), jnp.float32, 0.22, 0.5)
    token_positions = jnp.arange(SEQUENCE_LENGTH, dtype=jnp.int32)
    spike_events = jnp.zeros((SEQUENCE_COUNT, HEAD_COUNT, SEQUENCE_LENGTH), jnp.float32)
    for spike_event in range(3):
        spike_events = spike_events + jnp.where(token_positions[None, None, :] == spike_locations[:, :, spike_event:spike_event + 1], decay_amounts[:, :, spike_event:spike_event + 1], 0.0)
    gate_logarithm = -baseline_decay * block_multiplier * jitter_level - jnp.where(sluggish_head, spike_events, 0.0)
    return jnp.cumsum(gate_logarithm, axis=-1)


def levels(stream_key, shape, cuts, low, top_value):
    loudness = 1.0
    for dim, blocks in cuts:
        steps = jax.random.uniform(jax.random.fold_in(jax.random.fold_in(stream_key, 6), dim), (blocks,), jnp.float32, low / len(cuts), top_value / len(cuts))
        loudness = loudness * jnp.repeat(jnp.exp(steps), shape[dim] // blocks).reshape((-1,) + (1,) * (len(shape) - 1 - dim))
    return loudness


def normal_values(key, dims, scale, most, shards=(), kind=jnp.bfloat16):
    array = scale * jax.random.normal(key, dims, jnp.float32)
    if shards:
        array = array * levels(key, dims, shards, -0.22, 0.18)
    return jnp.clip(array, -most, most).astype(kind)


def setup_inputs(seed: int = 0) -> dict:
    key_list = jax.random.split(jax.random.key(seed), 6)
    queries = draw_queries(jax.random.fold_in(key_list[5], 71), 0)
    keys = draw_keys(jax.random.fold_in(key_list[5], 71), 0)
    values = draw_values(jax.random.fold_in(key_list[5], 71), 0)
    cum_gate = draw_cum_gate(jax.random.fold_in(key_list[5], 71), 0)
    out_weight = normal_values(key_list[4], (WIDTH, D), (WIDTH // 64) ** -0.5, 1.5, ((1, 8),))
    return {"queries": queries, "keys": keys, "values": values, "cum_gate": cum_gate, "out_weight": out_weight}


def reference(queries, keys, values, cum_gate, out_weight):
    sequences, length, width = queries.shape
    block_rows = min(512, length)
    block_count = length // block_rows
    score_scale = HEAD_DIM ** -0.5
    token_positions = jnp.arange(length, dtype=jnp.int32)

    def one_sequence(arrays):
        query_seq, key_seq, value_seq, gate_seq = arrays
        query_f = query_seq.astype(jnp.float32).reshape(length, HEAD_COUNT, HEAD_DIM)
        key_f = key_seq.astype(jnp.float32).reshape(length, HEAD_COUNT, HEAD_DIM)
        value_f = value_seq.astype(jnp.float32).reshape(length, HEAD_COUNT, HEAD_DIM)

        def one_block(block_index):
            first_row = (block_index * block_rows).astype(jnp.int32)
            query_part = lax.dynamic_slice_in_dim(query_f, first_row, block_rows, 0)
            gate_part = lax.dynamic_slice_in_dim(gate_seq, first_row, block_rows, 1)
            logits = jnp.einsum('qhe,khe->hqk', query_part, key_f) * score_scale
            logits = logits + gate_part[:, :, None] - gate_seq[:, None, :]
            query_rows = first_row + jnp.arange(block_rows, dtype=jnp.int32)
            allowed = token_positions[None, None, :] <= query_rows[None, :, None]
            logits = jnp.where(allowed, logits, -jnp.inf)
            scores = jnp.exp(logits - jnp.max(logits, axis=-1, keepdims=True))
            denominator = jnp.sum(scores, axis=-1)
            scores_low = lax.optimization_barrier(scores.astype(jnp.bfloat16)).astype(jnp.float32)
            weighted = jnp.einsum('hqk,khe->hqe', scores_low, value_f) / denominator[..., None]
            return weighted.transpose(1, 0, 2).reshape(block_rows, width).astype(jnp.bfloat16)

        blocks = lax.map(one_block, jnp.arange(block_count, dtype=jnp.int32))
        return blocks.reshape(length, width)

    attended = lax.map(one_sequence, (queries, keys, values, cum_gate))
    mixed = jnp.dot(attended.reshape(sequences * length, width), out_weight,
                    preferred_element_type=jnp.float32)
    return mixed.astype(jnp.bfloat16).reshape(sequences, length, out_weight.shape[1])
```

```python
import functools
import math

import jax
import jax.numpy as jnp
from jax import lax
from jax.experimental import pallas as pl
from jax.experimental.pallas import tpu as pltpu
from jax.sharding import PartitionSpec as P

LANES = 128
SUBLANES = 16
MESH = pl.DeviceIdType.MESH


def ring_index(position, n):
    upper = position // (n // 2)
    return (1 - upper) * (2 * position) + upper * (2 * (n - 1 - position) + 1)


def fused_kernel(
    sp, dp, depth, q, k, v, gate, w, tail, out,
    qg, kg, vg, og, attended, wg,
    qkv_send, qkv_recv, qkv_local, out_send, out_recv, out_local,
    ring_send, ring_recv, pair_send, pair_recv, own_sem,
):
    tokens, width = q.shape
    group = width // sp
    pairs = group // LANES
    per_pair = LANES // depth
    half_rows = width // 2
    main = wg.shape[3]
    rows = wg.shape[2]
    tail_rows = rows - half_rows
    columns = w.shape[1]
    tail_columns = columns - main
    steps = dp // 2
    cut = -(-(rows // 2) // SUBLANES) * SUBLANES
    me = lax.axis_index("sp")
    mine = lax.axis_index("dp")
    core = lax.rem(me, 2)
    partner = me + 1 - 2 * core
    odd = lax.rem(mine, 2)
    position = (1 - odd) * (mine // 2) + odd * (dp - 1 - mine // 2)
    right = ring_index(lax.rem(position + 1, dp), dp)
    left = ring_index(lax.rem(position + dp - 1, dp), dp)

    barrier = pltpu.get_barrier_semaphore()
    for d in range(1, sp):
        pl.semaphore_signal(
            barrier, inc=1, device_id=(lax.rem(me + d, sp), mine), device_id_type=MESH
        )
    for side in (left, right):
        pl.semaphore_signal(barrier, inc=1, device_id=(me, side), device_id_type=MESH)

    own_copies = []
    for half in range(2):
        own_copies.append(pltpu.make_async_copy(
            w.at[pl.ds(half * half_rows, half_rows), pl.ds(0, main)],
            wg.at[mine, half, pl.ds(0, half_rows)], own_sem.at[half]))
        own_copies.append(pltpu.make_async_copy(
            tail.at[half], wg.at[mine, half, pl.ds(half_rows, tail_rows)],
            own_sem.at[2 + half]))
    local_copies = {}
    arrays = ((q, qg), (k, kg), (v, vg))
    for p in range(pairs):
        for a, (source, target) in enumerate(arrays):
            local_copies[p, a] = pltpu.make_async_copy(
                source.at[:, pl.ds(pl.multiple_of(me * group + p * LANES, LANES), LANES)],
                target.at[p, pl.ds(pl.multiple_of(me * tokens, tokens), tokens), :],
                qkv_local.at[p, a])
    pl.semaphore_wait(barrier, sp + 1)

    qkv_copies = {}
    order = [2, 1, 3] if sp == 4 else list(range(1, sp))

    def send_pair(p):
        for a, (source, target) in enumerate(arrays):
            for d in order:
                peer = lax.rem(me + d, sp)
                copy = pltpu.make_async_remote_copy(
                    src_ref=source.at[:, pl.ds(pl.multiple_of(peer * group + p * LANES, LANES), LANES)],
                    dst_ref=target.at[p, pl.ds(pl.multiple_of(me * tokens, tokens), tokens), :],
                    send_sem=qkv_send.at[p, a, d - 1],
                    recv_sem=qkv_recv.at[p, a, d - 1],
                    device_id=(peer, mine),
                    device_id_type=MESH,
                )
                copy.start()
                qkv_copies[p, a, d] = copy

    ring_copies = {}
    pair_copies = {}

    def ring_slice(owner, side, step):
        if step < steps - 1:
            return wg.at[owner, core]
        if side == 0:
            return wg.at[owner, core, pl.ds(0, cut)]
        return wg.at[owner, core, pl.ds(cut, rows - cut)]

    def start_ring(key, source, target, side, slot):
        copy = pltpu.make_async_remote_copy(
            src_ref=source, dst_ref=target,
            send_sem=ring_send.at[side, slot], recv_sem=ring_recv.at[side, slot],
            device_id=(me, right if side == 0 else left), device_id_type=MESH)
        copy.start()
        ring_copies[key] = copy

    def ring_first():
        for side in range(2):
            start_ring((side, 0), w.at[pl.ds(pl.multiple_of(core * half_rows, half_rows), half_rows), pl.ds(0, main)],
                       wg.at[mine, core, pl.ds(0, half_rows)], side, 0)
            start_ring((side, steps), tail.at[core],
                       wg.at[mine, core, pl.ds(half_rows, tail_rows)], side, steps)

    def ring_step(step):
        for side in range(2):
            ring_copies[side, step].wait_recv()
            if step == 0:
                ring_copies[side, steps].wait_recv()
            shift = dp - 1 - step if side == 0 else 1 + step
            owner = ring_index(lax.rem(position + shift, dp), dp)
            if step + 1 < steps:
                piece = ring_slice(owner, side, step + 1)
                start_ring((side, step + 1), piece, piece, side, step + 1)
            piece = ring_slice(owner, side, step)
            copy = pltpu.make_async_remote_copy(
                src_ref=piece, dst_ref=piece,
                send_sem=pair_send.at[side, step], recv_sem=pair_recv.at[side, step],
                device_id=(partner, mine), device_id_type=MESH)
            copy.start()
            pair_copies[side, step] = copy

    send_pair(0)
    ring_first()
    for p in range(1, pairs):
        send_pair(p)
    for copy in local_copies.values():
        copy.start()
    for copy in own_copies:
        copy.start()

    log2e = math.log2(math.e)
    factor = depth ** -0.5 * log2e
    gates = gate[...] * log2e
    gates_t = jnp.transpose(gates)
    lane = lax.broadcasted_iota(jnp.int32, (tokens, LANES), 1) // depth
    diagonal = (
        lax.broadcasted_iota(jnp.int32, (tokens, tokens), 1)
        <= lax.broadcasted_iota(jnp.int32, (tokens, tokens), 0)
    )

    def attend_block(p, i):
        keys = (i + 1) * tokens
        query = qg[p, i * tokens:keys, :]
        key = kg[p, 0:keys, :]
        value = vg[p, 0:keys, :]
        result = jnp.zeros((tokens, LANES), jnp.float32)
        for j in range(per_pair):
            h = p * per_pair + j
            masked = jnp.where(lane == j, query, jnp.zeros_like(query))
            logits = lax.dot_general(
                masked, key, (((1,), (1,)), ((), ())), preferred_element_type=jnp.float32
            ) * factor
            logits = logits + (gates_t[i * tokens:keys, h:h + 1] - gates[h:h + 1, 0:keys])
            last = jnp.where(diagonal, logits[:, i * tokens:], -jnp.inf)
            logits = jnp.concatenate([logits[:, :i * tokens], last], axis=1) if i else last
            top = jnp.max(logits, axis=1, keepdims=True)
            scores = jnp.exp2(logits - top)
            total = jnp.sum(scores, axis=1, keepdims=True)
            weighted = jnp.dot(scores.astype(jnp.bfloat16), value, preferred_element_type=jnp.float32)
            result = jnp.where(lane == j, weighted / total, result)
        og[p, i * tokens:keys, :] = result.astype(jnp.bfloat16)

    out_copies = []

    def send_out(p):
        for d in order:
            peer = lax.rem(me + d, sp)
            copy = pltpu.make_async_remote_copy(
                src_ref=og.at[p, pl.ds(pl.multiple_of(peer * tokens, tokens), tokens), :],
                dst_ref=attended.at[:, pl.ds(pl.multiple_of(me * group + p * LANES, LANES), LANES)],
                send_sem=out_send.at[p, d - 1], recv_sem=out_recv.at[p, d - 1],
                device_id=(peer, mine), device_id_type=MESH)
            copy.start()
            out_copies.append(copy)
        copy = pltpu.make_async_copy(
            og.at[p, pl.ds(pl.multiple_of(me * tokens, tokens), tokens), :],
            attended.at[:, pl.ds(pl.multiple_of(me * group + p * LANES, LANES), LANES)],
            out_local.at[p])
        copy.start()
        own_copies.append(copy)

    done = 0
    for p in range(pairs):
        if done < steps:
            ring_step(done)
            done += 1
        for a in range(3):
            local_copies[p, a].wait()
            for d in order:
                qkv_copies[p, a, d].wait_recv()
        for i in range(sp):
            if i == sp // 2 and p == pairs - 1 and done < steps:
                ring_step(done)
                done += 1
            attend_block(p, i)
        send_out(p)
    while done < steps:
        ring_step(done)
        done += 1

    for copy in own_copies:
        copy.wait()
    for copy in out_copies:
        copy.wait()
    for copy in pair_copies.values():
        copy.wait()

    tail_first = jnp.zeros((tokens, dp * tail_rows), jnp.float32)
    tail_second = jnp.zeros((tokens, dp * tail_rows), jnp.float32)
    quarter = half_rows // 2
    nt = (((1,), (1,)), ((), ()))
    for half in range(2):
        packed = wg[:, half, half_rows:, :].reshape(dp * tail_rows, main)
        tail_first += lax.dot_general(
            attended[:, half * half_rows:half * half_rows + quarter], packed, nt,
            preferred_element_type=jnp.float32)
        tail_second += lax.dot_general(
            attended[:, half * half_rows + quarter:(half + 1) * half_rows], packed, nt,
            preferred_element_type=jnp.float32)
    for owner in range(dp):
        product = jnp.dot(
            attended[:, :half_rows], wg[owner, 0, :half_rows, :], preferred_element_type=jnp.float32)
        product += jnp.dot(
            attended[:, half_rows:], wg[owner, 1, :half_rows, :], preferred_element_type=jnp.float32)
        first = owner * tail_rows
        second = first + tail_columns
        end = (
            tail_first[:, first:first + tail_columns]
            + tail_second[:, second:second + tail_columns]
        )
        whole = jnp.concatenate([product, end], axis=1).astype(jnp.bfloat16)
        out[:, owner * columns:(owner + 1) * columns] = whole

    for copy in qkv_copies.values():
        copy.wait_send()
    for copy in ring_copies.values():
        copy.wait_send()


def fused(sp, dp, depth, q, k, v, gate, w):
    tokens, width = q.shape
    length = tokens * sp
    columns = w.shape[1]
    main = columns // LANES * LANES
    half = width // 2
    tail = w[:, main:].reshape(2, 2, half // 2, columns - main)
    tail = tail.transpose(0, 1, 3, 2).reshape(2, 2 * (columns - main), main)
    group = width // sp
    pairs = group // LANES
    steps = dp // 2
    any_spec = pl.BlockSpec(memory_space=pl.ANY)
    vmem_spec = pl.BlockSpec(memory_space=pltpu.VMEM)
    dma = pltpu.SemaphoreType.DMA
    gathered = pltpu.VMEM((pairs, length, LANES), jnp.bfloat16)
    return pl.pallas_call(
        functools.partial(fused_kernel, sp, dp, depth),
        out_shape=jax.ShapeDtypeStruct((tokens, columns * dp), jnp.bfloat16),
        in_specs=[any_spec, any_spec, any_spec, vmem_spec, any_spec, vmem_spec],
        out_specs=vmem_spec,
        scratch_shapes=[
            gathered, gathered, gathered, gathered,
            pltpu.VMEM((tokens, width), jnp.bfloat16),
            pltpu.VMEM((dp, 2, half + tail.shape[1], main), jnp.bfloat16),
            dma((pairs, 3, sp - 1)), dma((pairs, 3, sp - 1)), dma((pairs, 3)),
            dma((pairs, sp - 1)), dma((pairs, sp - 1)), dma((pairs,)),
            dma((2, steps + 1)), dma((2, steps + 1)),
            dma((2, steps)), dma((2, steps)), dma((4,)),
        ],
        compiler_params=pltpu.CompilerParams(
            collective_id=0, has_side_effects=True, vmem_limit_bytes=48 * 1024 * 1024),
    )(q, k, v, gate, w, tail)


def fits(sp, dp, tokens, width, depth, columns):
    main = columns // LANES * LANES
    return (
        sp % 2 == 0 and dp % 2 == 0 and dp >= 4
        and (width // sp) % LANES == 0 and LANES % depth == 0
        and tokens * sp <= 1024 and tokens % LANES == 0
        and main * 4 == width and columns > main
        and 2 * (columns - main) == SUBLANES
    )


def attend(query_all, key_all, value_all, gate_all):
    length, width = query_all.shape
    heads = gate_all.shape[0]
    depth = width // heads
    block_rows = min(512, length)
    block_count = length // block_rows
    score_scale = depth ** (-0.5)
    query_blocks = query_all.reshape(block_count, block_rows, heads, depth)
    key_blocks = key_all.reshape(block_count, block_rows, heads, depth)
    value_blocks = value_all.reshape(block_count, block_rows, heads, depth)
    gate_blocks = gate_all.reshape(heads, block_count, block_rows).transpose(1, 0, 2)
    offsets = jnp.arange(block_rows, dtype=jnp.int32)

    def one_block(block_index):
        query_part = lax.dynamic_index_in_dim(query_blocks, block_index, 0, keepdims=False)
        gate_part = lax.dynamic_index_in_dim(gate_blocks, block_index, 0, keepdims=False)
        query_rows = block_index * block_rows + offsets

        def key_step(key_block, carry):
            running_max, running_sum, weighted = carry
            key_part = lax.dynamic_index_in_dim(key_blocks, key_block, 0, keepdims=False)
            value_part = lax.dynamic_index_in_dim(value_blocks, key_block, 0, keepdims=False)
            gate_keys = lax.dynamic_index_in_dim(gate_blocks, key_block, 0, keepdims=False)
            logits = (
                jnp.einsum("qhe,khe->hqk", query_part, key_part, preferred_element_type=jnp.float32)
                * score_scale
            )
            logits = logits + gate_part[:, :, None] - gate_keys[:, None, :]
            key_rows = key_block * block_rows + offsets
            allowed = key_rows[None, :] <= query_rows[:, None]
            logits = jnp.where(allowed[None], logits, -jnp.inf)
            new_max = jnp.maximum(running_max, jnp.max(logits, axis=-1))
            scores = jnp.exp(logits - new_max[..., None])
            factor = jnp.exp(running_max - new_max)
            running_sum = running_sum * factor + jnp.sum(scores, axis=-1)
            weighted = weighted * factor[..., None] + jnp.einsum(
                "hqk,khe->hqe",
                scores.astype(jnp.bfloat16),
                value_part,
                preferred_element_type=jnp.float32,
            )
            return (new_max, running_sum, weighted)

        start_state = (
            jnp.full((heads, block_rows), -jnp.inf, jnp.float32),
            jnp.zeros((heads, block_rows), jnp.float32),
            jnp.zeros((heads, block_rows, depth), jnp.float32),
        )
        final_max, final_sum, weighted = lax.fori_loop(0, block_index + 1, key_step, start_state)
        result = weighted / final_sum[..., None]
        return result.transpose(1, 0, 2).astype(jnp.bfloat16)

    outputs = lax.map(one_block, jnp.arange(block_count, dtype=jnp.int32))
    return outputs.reshape(length, width)


def body(queries, keys, values, cum_gate, out_weight):
    sp, dp = lax.axis_size("sp"), lax.axis_size("dp")
    tokens, width = queries.shape[1:]
    depth = width // (cum_gate.shape[1] * sp)
    if fits(sp, dp, tokens, width, depth, out_weight.shape[1]):
        mixed = fused(sp, dp, depth, queries[0], keys[0], values[0], cum_gate[0], out_weight)
        return mixed[None]
    query_heads, key_heads, value_heads = (
        lax.all_to_all(queries, "sp", split_axis=2, concat_axis=1, tiled=True),
        lax.all_to_all(keys, "sp", split_axis=2, concat_axis=1, tiled=True),
        lax.all_to_all(values, "sp", split_axis=2, concat_axis=1, tiled=True),
    )
    local_out = attend(query_heads[0], key_heads[0], value_heads[0], cum_gate[0])
    attended = lax.all_to_all(local_out[None], "sp", split_axis=1, concat_axis=2, tiled=True)[0]
    group_rows = attended.shape[1] // lax.axis_size("sp")
    own_rows = lax.dynamic_slice_in_dim(
        out_weight, lax.axis_index("sp") * group_rows, group_rows, 0
    )
    full_rows = lax.all_gather(own_rows, "dp", axis=1, tiled=True)
    whole_weight = lax.all_gather(full_rows, "sp", axis=0, tiled=True)
    mixed = jnp.dot(attended, whole_weight, preferred_element_type=jnp.float32)
    return mixed.astype(jnp.bfloat16)[None]


def solution(mesh):
    in_specs = (
        P("dp", "sp", None),
        P("dp", "sp", None),
        P("dp", "sp", None),
        P("dp", "sp", None),
        P(None, "dp"),
    )
    out_specs = P("dp", "sp", None)
    return jax.shard_map(body, mesh=mesh, in_specs=in_specs, out_specs=out_specs, check_vma=False)
```

```python
import functools
import math

import jax
import jax.numpy as jnp
from jax import lax
from jax.experimental import pallas as pl
from jax.experimental.pallas import tpu as pltpu
from jax.sharding import PartitionSpec as P

LANES = 128
SUBLANES = 16
MESH = pl.DeviceIdType.MESH


def ring_index(position, n):
    upper = position // (n // 2)
    return (1 - upper) * (2 * position) + upper * (2 * (n - 1 - position) + 1)


def fused_kernel(
    dp, depth, q, k, v, gate, w, out,
    qg, kg, vg, qx, local_f32, local_stats, ox, orx, sx, srx, done_out, attended, gates_all, wfull, wg,
    gate_send, gate_recv, swap_send, swap_recv, swap_local, qx_send, qx_recv,
    ox_send, ox_recv, sx_send, sx_recv, fin_send, fin_recv, fin_local,
    ring_send, ring_recv, pair_send, pair_recv, own_sem,
):
    tokens, width = q.shape
    group = width // 2
    chip_rows = 2 * tokens
    pairs = group // LANES
    per_pair = LANES // depth
    half_rows = width // 2
    main = wg.shape[3]
    rows = wg.shape[2]
    tail_rows = rows - half_rows
    columns = w.shape[1]
    tail_columns = columns - main
    steps = dp // 2
    cut = -(-(rows // 2) // SUBLANES) * SUBLANES
    me = lax.axis_index("sp")
    mine = lax.axis_index("dp")
    core = lax.rem(me, 2)
    chip = me // 2
    partner = me + 1 - 2 * core
    odd = lax.rem(mine, 2)
    position = (1 - odd) * (mine // 2) + odd * (dp - 1 - mine // 2)
    right = ring_index(lax.rem(position + 1, dp), dp)
    left = ring_index(lax.rem(position + dp - 1, dp), dp)

    def remote(source, target, send, recv, sp_index, dp_index):
        return pltpu.make_async_remote_copy(
            src_ref=source, dst_ref=target, send_sem=send, recv_sem=recv,
            device_id=(sp_index, dp_index), device_id_type=MESH)

    def aligned(index, size):
        return pl.ds(pl.multiple_of(index * size, size), size)

    barrier = pltpu.get_barrier_semaphore()
    for d in range(1, 4):
        pl.semaphore_signal(
            barrier, inc=1, device_id=(lax.rem(me + d, 4), mine), device_id_type=MESH
        )
    for side in (left, right):
        pl.semaphore_signal(barrier, inc=1, device_id=(me, side), device_id_type=MESH)

    whole_w = pltpu.make_async_copy(w, wfull, own_sem.at[0])
    whole_w.start()
    own_copies = [
        pltpu.make_async_copy(
            w.at[pl.ds(half * half_rows, half_rows), pl.ds(0, main)],
            wg.at[mine, half, pl.ds(0, half_rows)], own_sem.at[1 + half])
        for half in range(2)
    ]
    arrays = ((q, qg), (k, kg), (v, vg))
    swap_copies, local_copies = [], []
    for a, (source, target) in enumerate(arrays):
        swap_copies.append(remote(
            source.at[:, aligned(1 - core, group)], target.at[aligned(core, tokens), :],
            swap_send.at[a], swap_recv.at[a], partner, mine))
        local_copies.append(pltpu.make_async_copy(
            source.at[:, aligned(core, group)], target.at[aligned(core, tokens), :], swap_local.at[a]))
    gate_copies = [
        remote(gate, gates_all.at[me], gate_send.at[d - 1], gate_recv.at[d - 1],
               lax.rem(me + d, 4), mine)
        for d in range(1, 4)
    ]
    query_sends = {
        (p, a): remote(
            q.at[:, pl.ds(a * group + p * LANES, LANES)],
            qx.at[aligned(core, tokens), pl.ds(p * LANES, LANES)],
            qx_send.at[p, a], qx_recv.at[p, core], a, mine)
        for p in range(pairs) for a in range(2)
    }
    query_recvs = {
        (p, c): remote(
            q.at[:, pl.ds(p * LANES, LANES)],
            qx.at[pl.ds(c * tokens, tokens), pl.ds(p * LANES, LANES)],
            qx_send.at[p, c], qx_recv.at[p, c], partner, mine)
        for p in range(pairs) for c in range(2)
    }
    across = lax.rem(me + 2, 4)
    cross_sends = {
        (p, i): remote(
            ox.at[pl.ds(i * tokens, tokens), pl.ds(p * LANES, LANES)],
            orx.at[pl.ds(i * tokens, tokens), pl.ds(p * LANES, LANES)],
            ox_send.at[p, i], ox_recv.at[p, i], across, mine)
        for p in range(pairs) for i in range(2)
    }
    stat_sends = {
        (p, i): remote(sx.at[p, i], srx.at[p, i], sx_send.at[p, i], sx_recv.at[p, i], across, mine)
        for p in range(pairs) for i in range(2)
    }
    final_copy = remote(
        done_out.at[aligned(1 - core, tokens), :], attended.at[:, aligned(core, group)],
        fin_send.at[0], fin_recv.at[0], partner, mine)
    final_local = pltpu.make_async_copy(
        done_out.at[aligned(core, tokens), :], attended.at[:, aligned(core, group)], fin_local.at[0])

    spans = ((0, cut), (cut, rows - cut))
    ring, swap_weight = {}, {}
    for side in range(2):
        target = right if side == 0 else left
        for step in range(steps):
            shift = lax.rem(position + (dp - step if side == 0 else step), dp)
            sent = ring_index(shift, dp)
            shift = lax.rem(position + (dp - 1 - step if side == 0 else 1 + step), dp)
            came = ring_index(shift, dp)
            for piece, (start, size) in enumerate(spans):
                if step == steps - 1 and piece != side:
                    continue
                span = pl.ds(start, size)
                source = wg.at[sent, core, span]
                if step == 0:
                    if piece == 1:
                        span = pl.ds(start, size - tail_rows)
                        size -= tail_rows
                    source = w.at[pl.ds(pl.multiple_of(core * half_rows + start, SUBLANES), size), pl.ds(0, main)]
                ring[side, step, piece] = remote(
                    source, wg.at[sent, core, span],
                    ring_send.at[side, step, piece], ring_recv.at[side, step, piece], me, target)
                span = pl.ds(start, spans[piece][1])
                swap_weight[side, step, piece] = remote(
                    wg.at[came, core, span], wg.at[came, core, span],
                    pair_send.at[side, step, piece], pair_recv.at[side, step, piece], partner, mine)
        span = pl.ds(half_rows, tail_rows)
        ring[side, "tail"] = remote(
            wg.at[mine, core, span], wg.at[mine, core, span],
            ring_send.at[side, steps, 0], ring_recv.at[side, steps, 0], me, target)

    events = [(step, piece) for step in range(steps - 1) for piece in range(2)]

    def ring_event(n):
        if n < len(events):
            step, piece = events[n]
            for side in range(2):
                ring[side, step, piece].wait_recv()
                if step == 0 and piece == 1:
                    ring[side, "tail"].wait_recv()
                if (side, step + 1, piece) in ring:
                    ring[side, step + 1, piece].start()
                swap_weight[side, step, piece].start()
        elif n == len(events):
            for side in range(2):
                ring[side, steps - 1, side].wait_recv()
                swap_weight[side, steps - 1, side].start()

    pl.semaphore_wait(barrier, 5)
    for copy in gate_copies + swap_copies:
        copy.start()

    @pl.when(chip == 1)
    def _():
        for p in range(pairs):
            for a in range(2):
                query_sends[p, a].start()

    for piece in range(2):
        for side in range(2):
            ring[side, 0, piece].start()
    for copy in local_copies + own_copies:
        copy.start()
    gates_all[me] = gate[...]

    whole_w.wait()
    quarter = half_rows // 2
    nt = (((1,), (1,)), ((), ()))
    picked = lax.broadcasted_iota(jnp.int32, (tail_rows, tail_columns), 0)
    column = lax.broadcasted_iota(jnp.int32, (tail_rows, tail_columns), 1)
    for half in range(2):
        packed = jnp.zeros((tail_rows, quarter), jnp.float32)
        for a in range(2):
            chosen = jnp.where(picked == column + a * tail_columns, 1.0, 0.0).astype(jnp.bfloat16)
            first = half * half_rows + a * quarter
            packed += lax.dot_general(
                chosen, wfull[first:first + quarter, main:], nt, preferred_element_type=jnp.float32)
        wg[mine, half, half_rows:, :] = packed.astype(jnp.bfloat16)
    for side in range(2):
        ring[side, "tail"].start()

    log2e = math.log2(math.e)
    factor = depth ** -0.5 * log2e
    lane = lax.broadcasted_iota(jnp.int32, (tokens, LANES), 1)
    head_lane = lane // depth
    diagonal = (
        lax.broadcasted_iota(jnp.int32, (tokens, tokens), 1)
        <= lax.broadcasted_iota(jnp.int32, (tokens, tokens), 0)
    )
    heads_held = gates_all.shape[1]

    def block(p, query, keys, causal, query_first, key_first):
        key = kg[0:keys, p * LANES:(p + 1) * LANES]
        value = vg[0:keys, p * LANES:(p + 1) * LANES]
        holder = core * 2 + p * per_pair // heads_held
        query_gates = jnp.transpose(gates_all[holder, :, query_first:query_first + tokens]) * log2e
        key_gates = gates_all[holder, :, key_first:key_first + keys] * log2e
        parts = []
        for j in range(per_pair):
            h = p * per_pair % heads_held + j
            masked = jnp.where(head_lane == j, query, jnp.zeros_like(query))
            logits = lax.dot_general(masked, key, nt, preferred_element_type=jnp.float32) * factor
            logits = logits + (query_gates[:, h:h + 1] - key_gates[h:h + 1, :])
            if causal:
                last = jnp.where(diagonal, logits[:, keys - tokens:], -jnp.inf)
                logits = jnp.concatenate([logits[:, :keys - tokens], last], axis=1) if keys > tokens else last
            top = jnp.max(logits, axis=1, keepdims=True)
            scores = jnp.exp2(logits - top)
            total = jnp.sum(scores, axis=1, keepdims=True)
            weighted = jnp.dot(scores.astype(jnp.bfloat16), value, preferred_element_type=jnp.float32)
            parts.append((weighted, top, total))
        return parts

    def by_head(values):
        result = values[0]
        for j in range(1, per_pair):
            result = jnp.where(head_lane == j, values[j], result)
        return result

    def stats_of(parts):
        result = jnp.zeros((tokens, LANES), jnp.float32)
        for j, (_, top, total) in enumerate(parts):
            result = jnp.where(lane == j, top, result)
            result = jnp.where(lane == per_pair + j, total, result)
        return result

    def wait_swapped():
        for copy in local_copies:
            copy.wait()
        for copy in swap_copies + gate_copies:
            copy.wait_recv()

    def pair_columns(p):
        return slice(p * LANES, (p + 1) * LANES)

    @pl.when(chip == 0)
    def _():
        wait_swapped()
        for p in range(pairs):
            for i in range(2):
                first = i * tokens
                parts = block(p, qg[first:first + tokens, pair_columns(p)], first + tokens, True, first, 0)
                done_out[first:first + tokens, pair_columns(p)] = by_head(
                    [weighted / total for weighted, _, total in parts]).astype(jnp.bfloat16)
            if p == pairs // 2 - 1:
                ring_event(0)
        final_copy.start()
        final_local.start()
        ring_event(1)
        for p in range(pairs):
            if p == pairs // 2:
                ring_event(2)
            for c in range(2):
                query_recvs[p, c].wait_recv()
            for i in range(2):
                first = i * tokens
                parts = block(
                    p, qx[first:first + tokens, pair_columns(p)], chip_rows, False, chip_rows + first, 0)
                ox[first:first + tokens, pair_columns(p)] = by_head(
                    [weighted / total for weighted, _, total in parts]).astype(jnp.bfloat16)
                sx[p, i] = jnp.transpose(stats_of(parts))[:8, :]
                cross_sends[p, i].start()
                stat_sends[p, i].start()
        ring_event(3)
        ring_event(4)
        for copy in list(cross_sends.values()) + list(stat_sends.values()):
            copy.wait_send()

    @pl.when(chip == 1)
    def _():
        wait_swapped()
        for p in range(pairs):
            for i in range(2):
                first = i * tokens
                parts = block(
                    p, qg[first:first + tokens, pair_columns(p)], first + tokens, True,
                    chip_rows + first, chip_rows)
                local_f32[first:first + tokens, pair_columns(p)] = by_head([part[0] for part in parts])
                local_stats[p, first:first + tokens, :] = stats_of(parts)
            if p == pairs // 2 - 1:
                ring_event(0)
        ring_event(1)
        for p in range(pairs):
            if p == 1:
                ring_event(2)
            if p == 2:
                ring_event(3)
            if p == 3:
                ring_event(4)
            for i in range(2):
                first = i * tokens
                cross_sends[p, i].wait_recv()
                stat_sends[p, i].wait_recv()
                far_stats = jnp.transpose(srx[p, i])
                near_stats = local_stats[p, first:first + tokens, :]
                near, far, total = [], [], []
                for j in range(per_pair):
                    near_top, far_top = near_stats[:, j:j + 1], far_stats[:, j:j + 1]
                    top = jnp.maximum(near_top, far_top)
                    near_factor = jnp.exp2(near_top - top)
                    far_factor = jnp.exp2(far_top - top) * far_stats[:, per_pair + j:per_pair + j + 1]
                    total = near_factor * near_stats[:, per_pair + j:per_pair + j + 1] + far_factor
                    near.append(near_factor / total)
                    far.append(far_factor / total)
                merged = (
                    local_f32[first:first + tokens, pair_columns(p)] * by_head(near)
                    + orx[first:first + tokens, pair_columns(p)].astype(jnp.float32) * by_head(far)
                )
                done_out[first:first + tokens, pair_columns(p)] = merged.astype(jnp.bfloat16)
        final_copy.start()
        final_local.start()
        for copy in query_sends.values():
            copy.wait_send()

    for n in range(5, len(events) + 1):
        ring_event(n)

    for copy in own_copies:
        copy.wait()
    final_local.wait()
    final_copy.wait()
    for copy in swap_weight.values():
        copy.wait()

    tail_first = jnp.zeros((tokens, dp * tail_rows), jnp.float32)
    tail_second = jnp.zeros((tokens, dp * tail_rows), jnp.float32)
    for half in range(2):
        packed = wg[:, half, half_rows:, :].reshape(dp * tail_rows, main)
        tail_first += lax.dot_general(
            attended[:, half * half_rows:half * half_rows + quarter], packed, nt,
            preferred_element_type=jnp.float32)
        tail_second += lax.dot_general(
            attended[:, half * half_rows + quarter:(half + 1) * half_rows], packed, nt,
            preferred_element_type=jnp.float32)
    for owner in range(dp):
        product = jnp.dot(
            attended[:, :half_rows], wg[owner, 0, :half_rows, :], preferred_element_type=jnp.float32)
        product += jnp.dot(
            attended[:, half_rows:], wg[owner, 1, :half_rows, :], preferred_element_type=jnp.float32)
        first = owner * tail_rows
        second = first + tail_columns
        end = (
            tail_first[:, first:first + tail_columns]
            + tail_second[:, second:second + tail_columns]
        )
        whole = jnp.concatenate([product, end], axis=1).astype(jnp.bfloat16)
        out[:, owner * columns:(owner + 1) * columns] = whole

    for copy in gate_copies + swap_copies + list(ring.values()):
        copy.wait_send()


def fused(dp, depth, q, k, v, gate, w):
    tokens, width = q.shape
    columns = w.shape[1]
    main = columns // LANES * LANES
    half = width // 2
    pairs = half // LANES
    steps = dp // 2
    any_spec = pl.BlockSpec(memory_space=pl.ANY)
    vmem_spec = pl.BlockSpec(memory_space=pltpu.VMEM)
    dma = pltpu.SemaphoreType.DMA
    held = pltpu.VMEM((2 * tokens, half), jnp.bfloat16)
    stats = pltpu.VMEM((pairs, 2, 8, tokens), jnp.float32)
    return pl.pallas_call(
        functools.partial(fused_kernel, dp, depth),
        out_shape=jax.ShapeDtypeStruct((tokens, columns * dp), jnp.bfloat16),
        in_specs=[any_spec, any_spec, any_spec, vmem_spec, any_spec],
        out_specs=vmem_spec,
        scratch_shapes=[
            held, held, held, held,
            pltpu.VMEM((2 * tokens, half), jnp.float32),
            pltpu.VMEM((pairs, 2 * tokens, LANES), jnp.float32),
            held, held, stats, stats, held,
            pltpu.VMEM((tokens, width), jnp.bfloat16),
            pltpu.VMEM((4,) + gate.shape, jnp.float32),
            pltpu.VMEM(w.shape, jnp.bfloat16),
            pltpu.VMEM((dp, 2, half + SUBLANES, main), jnp.bfloat16),
            dma((3,)), dma((3,)), dma((3,)), dma((3,)), dma((3,)),
            dma((pairs, 2)), dma((pairs, 2)),
            dma((pairs, 2)), dma((pairs, 2)), dma((pairs, 2)), dma((pairs, 2)),
            dma((1,)), dma((1,)), dma((1,)),
            dma((2, steps + 1, 2)), dma((2, steps + 1, 2)),
            dma((2, steps, 2)), dma((2, steps, 2)), dma((3,)),
        ],
        compiler_params=pltpu.CompilerParams(
            collective_id=0, has_side_effects=True, vmem_limit_bytes=48 * 1024 * 1024),
    )(q, k, v, gate, w)


def fits(sp, dp, tokens, width, depth, columns):
    main = columns // LANES * LANES
    return (
        sp == 4 and dp % 2 == 0 and 8 <= dp <= 16
        and width % (2 * LANES) == 0 and width <= 1024 and LANES % depth == 0
        and tokens <= 256 and tokens % LANES == 0
        and (width // depth // sp) % (LANES // depth) == 0
        and LANES // depth <= 4
        and main * 4 == width and columns > main
        and 2 * (columns - main) == SUBLANES
    )


def attend(query_all, key_all, value_all, gate_all):
    length, width = query_all.shape
    heads = gate_all.shape[0]
    depth = width // heads
    block_rows = min(512, length)
    block_count = length // block_rows
    score_scale = depth ** (-0.5)
    query_blocks = query_all.reshape(block_count, block_rows, heads, depth)
    key_blocks = key_all.reshape(block_count, block_rows, heads, depth)
    value_blocks = value_all.reshape(block_count, block_rows, heads, depth)
    gate_blocks = gate_all.reshape(heads, block_count, block_rows).transpose(1, 0, 2)
    offsets = jnp.arange(block_rows, dtype=jnp.int32)

    def one_block(block_index):
        query_part = lax.dynamic_index_in_dim(query_blocks, block_index, 0, keepdims=False)
        gate_part = lax.dynamic_index_in_dim(gate_blocks, block_index, 0, keepdims=False)
        query_rows = block_index * block_rows + offsets

        def key_step(key_block, carry):
            running_max, running_sum, weighted = carry
            key_part = lax.dynamic_index_in_dim(key_blocks, key_block, 0, keepdims=False)
            value_part = lax.dynamic_index_in_dim(value_blocks, key_block, 0, keepdims=False)
            gate_keys = lax.dynamic_index_in_dim(gate_blocks, key_block, 0, keepdims=False)
            logits = (
                jnp.einsum("qhe,khe->hqk", query_part, key_part, preferred_element_type=jnp.float32)
                * score_scale
            )
            logits = logits + gate_part[:, :, None] - gate_keys[:, None, :]
            key_rows = key_block * block_rows + offsets
            allowed = key_rows[None, :] <= query_rows[:, None]
            logits = jnp.where(allowed[None], logits, -jnp.inf)
            new_max = jnp.maximum(running_max, jnp.max(logits, axis=-1))
            scores = jnp.exp(logits - new_max[..., None])
            factor = jnp.exp(running_max - new_max)
            running_sum = running_sum * factor + jnp.sum(scores, axis=-1)
            weighted = weighted * factor[..., None] + jnp.einsum(
                "hqk,khe->hqe",
                scores.astype(jnp.bfloat16),
                value_part,
                preferred_element_type=jnp.float32,
            )
            return (new_max, running_sum, weighted)

        start_state = (
            jnp.full((heads, block_rows), -jnp.inf, jnp.float32),
            jnp.zeros((heads, block_rows), jnp.float32),
            jnp.zeros((heads, block_rows, depth), jnp.float32),
        )
        final_max, final_sum, weighted = lax.fori_loop(0, block_index + 1, key_step, start_state)
        result = weighted / final_sum[..., None]
        return result.transpose(1, 0, 2).astype(jnp.bfloat16)

    outputs = lax.map(one_block, jnp.arange(block_count, dtype=jnp.int32))
    return outputs.reshape(length, width)


def body(queries, keys, values, cum_gate, out_weight):
    sp, dp = lax.axis_size("sp"), lax.axis_size("dp")
    tokens, width = queries.shape[1:]
    depth = width // (cum_gate.shape[1] * sp)
    if fits(sp, dp, tokens, width, depth, out_weight.shape[1]):
        mixed = fused(dp, depth, queries[0], keys[0], values[0], cum_gate[0], out_weight)
        return mixed[None]
    query_heads, key_heads, value_heads = (
        lax.all_to_all(queries, "sp", split_axis=2, concat_axis=1, tiled=True),
        lax.all_to_all(keys, "sp", split_axis=2, concat_axis=1, tiled=True),
        lax.all_to_all(values, "sp", split_axis=2, concat_axis=1, tiled=True),
    )
    local_out = attend(query_heads[0], key_heads[0], value_heads[0], cum_gate[0])
    attended = lax.all_to_all(local_out[None], "sp", split_axis=1, concat_axis=2, tiled=True)[0]
    group_rows = attended.shape[1] // lax.axis_size("sp")
    own_rows = lax.dynamic_slice_in_dim(
        out_weight, lax.axis_index("sp") * group_rows, group_rows, 0
    )
    full_rows = lax.all_gather(own_rows, "dp", axis=1, tiled=True)
    whole_weight = lax.all_gather(full_rows, "sp", axis=0, tiled=True)
    mixed = jnp.dot(attended, whole_weight, preferred_element_type=jnp.float32)
    return mixed.astype(jnp.bfloat16)[None]


def solution(mesh):
    in_specs = (
        P("dp", "sp", None),
        P("dp", "sp", None),
        P("dp", "sp", None),
        P("dp", "sp", None),
        P(None, "dp"),
    )
    out_specs = P("dp", "sp", None)
    return jax.shard_map(body, mesh=mesh, in_specs=in_specs, out_specs=out_specs, check_vma=False)
```

```python
import functools
import math

import jax
import jax.numpy as jnp
from jax import lax
from jax.experimental import pallas as pl
from jax.experimental.pallas import tpu as pltpu
from jax.sharding import PartitionSpec as P

LANES = 128
MESH = pl.DeviceIdType.MESH


def ring_index(position, n):
    upper = position // (n // 2)
    return (1 - upper) * (2 * position) + upper * (2 * (n - 1 - position) + 1)


def fused_kernel(
    dp, depth, q, k, v, gate, w, out,
    qg, kg, vg, qx, local_f32, local_stats, ox, orx, sx, srx, done_out, attended, gates_all, wg,
    gate_send, gate_recv, swap_send, swap_recv, swap_local, qx_send, qx_recv,
    ox_send, ox_recv, sx_send, sx_recv, fin_send, fin_recv, fin_local,
    ring_send, ring_recv, pair_send, pair_recv, own_sem,
):
    tokens, width = q.shape
    group = width // 2
    chip_rows = 2 * tokens
    pairs = group // LANES
    per_pair = LANES // depth
    quarter = width // 4
    columns = w.shape[0]
    steps = dp // 2
    me = lax.axis_index("sp")
    mine = lax.axis_index("dp")
    core = lax.rem(me, 2)
    chip = me // 2
    partner = me + 1 - 2 * core
    odd = lax.rem(mine, 2)
    position = (1 - odd) * (mine // 2) + odd * (dp - 1 - mine // 2)
    right = ring_index(lax.rem(position + 1, dp), dp)
    left = ring_index(lax.rem(position + dp - 1, dp), dp)

    def remote(source, target, send, recv, sp_index, dp_index):
        return pltpu.make_async_remote_copy(
            src_ref=source, dst_ref=target, send_sem=send, recv_sem=recv,
            device_id=(sp_index, dp_index), device_id_type=MESH)

    def aligned(index, size):
        return pl.ds(pl.multiple_of(index * size, size), size)

    barrier = pltpu.get_barrier_semaphore()
    for d in range(1, 4):
        pl.semaphore_signal(
            barrier, inc=1, device_id=(lax.rem(me + d, 4), mine), device_id_type=MESH
        )
    for side in (left, right):
        pl.semaphore_signal(barrier, inc=1, device_id=(me, side), device_id_type=MESH)

    own_copies = [
        pltpu.make_async_copy(w.at[:, pl.ds(n * quarter, quarter)], wg.at[mine, n], own_sem.at[n])
        for n in range(4)
    ]
    arrays = ((q, qg), (k, kg), (v, vg))
    swap_copies, local_copies = [], []
    for a, (source, target) in enumerate(arrays):
        swap_copies.append(remote(
            source.at[:, aligned(1 - core, group)], target.at[aligned(core, tokens), :],
            swap_send.at[a], swap_recv.at[a], partner, mine))
        local_copies.append(pltpu.make_async_copy(
            source.at[:, aligned(core, group)], target.at[aligned(core, tokens), :], swap_local.at[a]))
    gate_copies = [
        remote(gate, gates_all.at[me], gate_send.at[d - 1], gate_recv.at[d - 1],
               lax.rem(me + d, 4), mine)
        for d in range(1, 4)
    ]
    query_sends = {
        (p, a): remote(
            q.at[:, pl.ds(a * group + p * LANES, LANES)],
            qx.at[aligned(core, tokens), pl.ds(p * LANES, LANES)],
            qx_send.at[p, a], qx_recv.at[p, core], a, mine)
        for p in range(pairs) for a in range(2)
    }
    query_recvs = {
        (p, c): remote(
            q.at[:, pl.ds(p * LANES, LANES)],
            qx.at[pl.ds(c * tokens, tokens), pl.ds(p * LANES, LANES)],
            qx_send.at[p, c], qx_recv.at[p, c], partner, mine)
        for p in range(pairs) for c in range(2)
    }
    across = lax.rem(me + 2, 4)
    cross_sends = {
        (p, i): remote(
            ox.at[pl.ds(i * tokens, tokens), pl.ds(p * LANES, LANES)],
            orx.at[pl.ds(i * tokens, tokens), pl.ds(p * LANES, LANES)],
            ox_send.at[p, i], ox_recv.at[p, i], across, mine)
        for p in range(pairs) for i in range(2)
    }
    stat_sends = {
        (p, i): remote(sx.at[p, i], srx.at[p, i], sx_send.at[p, i], sx_recv.at[p, i], across, mine)
        for p in range(pairs) for i in range(2)
    }
    final_copy = remote(
        done_out.at[aligned(1 - core, tokens), :], attended.at[:, aligned(core, group)],
        fin_send.at[0], fin_recv.at[0], partner, mine)
    final_local = pltpu.make_async_copy(
        done_out.at[aligned(core, tokens), :], attended.at[:, aligned(core, group)], fin_local.at[0])

    ring, swap_weight, came_from = {}, {}, {}
    for side in range(2):
        target = right if side == 0 else left
        for step in range(steps):
            shift = lax.rem(position + (dp - step if side == 0 else step), dp)
            sent = ring_index(shift, dp)
            shift = lax.rem(position + (dp - 1 - step if side == 0 else 1 + step), dp)
            came = ring_index(shift, dp)
            came_from[side, step] = came
            for piece in range(2):
                if step == steps - 1 and piece != side:
                    continue
                place = 2 * core + piece
                source = wg.at[sent, place] if step else w.at[:, aligned(place, quarter)]
                ring[side, step, piece] = remote(
                    source, wg.at[sent, place],
                    ring_send.at[side, step, piece], ring_recv.at[side, step, piece], me, target)
                swap_weight[side, step, piece] = remote(
                    wg.at[came, place], wg.at[came, place],
                    pair_send.at[side, step, piece], pair_recv.at[side, step, piece], partner, mine)

    events = [(step, piece) for step in range(steps - 1) for piece in range(2)]

    def ring_event(n):
        if n < len(events):
            step, piece = events[n]
            for side in range(2):
                ring[side, step, piece].wait_recv()
                if (side, step + 1, piece) in ring:
                    ring[side, step + 1, piece].start()
                swap_weight[side, step, piece].start()
        elif n == len(events):
            for side in range(2):
                ring[side, steps - 1, side].wait_recv()
                swap_weight[side, steps - 1, side].start()

    pl.semaphore_wait(barrier, 5)
    for side in range(2):
        ring[side, 0, 0].start()

    @pl.when(chip == 1)
    def _():
        for a in range(2):
            query_sends[0, a].start()

    for copy in gate_copies + swap_copies:
        copy.start()

    @pl.when(chip == 1)
    def _():
        for p in range(1, pairs):
            for a in range(2):
                query_sends[p, a].start()

    for side in range(2):
        ring[side, 0, 1].start()
    for copy in local_copies + own_copies:
        copy.start()
    gates_all[me] = gate[...]

    nt = (((1,), (1,)), ((), ()))
    log2e = math.log2(math.e)
    factor = depth ** -0.5 * log2e
    lane = lax.broadcasted_iota(jnp.int32, (tokens, LANES), 1)
    head_lane = lane // depth
    diagonal = (
        lax.broadcasted_iota(jnp.int32, (tokens, tokens), 1)
        <= lax.broadcasted_iota(jnp.int32, (tokens, tokens), 0)
    )
    heads_held = gates_all.shape[1]

    def block(p, query, keys, causal, query_first, key_first):
        key = kg[0:keys, p * LANES:(p + 1) * LANES]
        value = vg[0:keys, p * LANES:(p + 1) * LANES]
        holder = core * 2 + p * per_pair // heads_held
        query_gates = jnp.transpose(gates_all[holder, :, query_first:query_first + tokens]) * log2e
        key_gates = gates_all[holder, :, key_first:key_first + keys] * log2e
        parts = []
        for j in range(per_pair):
            h = p * per_pair % heads_held + j
            masked = jnp.where(head_lane == j, query, jnp.zeros_like(query))
            logits = lax.dot_general(masked, key, nt, preferred_element_type=jnp.float32) * factor
            logits = logits + (query_gates[:, h:h + 1] - key_gates[h:h + 1, :])
            if causal:
                last = jnp.where(diagonal, logits[:, keys - tokens:], -jnp.inf)
                logits = jnp.concatenate([logits[:, :keys - tokens], last], axis=1) if keys > tokens else last
            top = jnp.max(logits, axis=1, keepdims=True)
            scores = jnp.exp2(logits - top)
            total = jnp.sum(scores, axis=1, keepdims=True)
            weighted = jnp.dot(scores.astype(jnp.bfloat16), value, preferred_element_type=jnp.float32)
            parts.append((weighted, top, total))
        return parts

    def by_head(values):
        result = values[0]
        for j in range(1, per_pair):
            result = jnp.where(head_lane == j, values[j], result)
        return result

    def stats_of(parts):
        result = jnp.zeros((tokens, LANES), jnp.float32)
        for j, (_, top, total) in enumerate(parts):
            result = jnp.where(lane == j, top, result)
            result = jnp.where(lane == per_pair + j, total, result)
        return result

    def wait_swapped():
        for copy in local_copies:
            copy.wait()
        for copy in swap_copies + gate_copies:
            copy.wait_recv()

    def pair_columns(p):
        return slice(p * LANES, (p + 1) * LANES)

    @pl.when(chip == 0)
    def _():
        wait_swapped()
        for p in range(pairs):
            for i in range(2):
                first = i * tokens
                parts = block(p, qg[first:first + tokens, pair_columns(p)], first + tokens, True, first, 0)
                done_out[first:first + tokens, pair_columns(p)] = by_head(
                    [weighted / total for weighted, _, total in parts]).astype(jnp.bfloat16)
        final_copy.start()
        final_local.start()
        ring_event(0)
        for p in range(pairs):
            if p == pairs // 2:
                ring_event(1)
            for c in range(2):
                query_recvs[p, c].wait_recv()
            for i in range(2):
                first = i * tokens
                parts = block(
                    p, qx[first:first + tokens, pair_columns(p)], chip_rows, False, chip_rows + first, 0)
                ox[first:first + tokens, pair_columns(p)] = by_head(
                    [weighted / total for weighted, _, total in parts]).astype(jnp.bfloat16)
                sx[p, i] = jnp.transpose(stats_of(parts))[:8, :]
                cross_sends[p, i].start()
                stat_sends[p, i].start()
        ring_event(2)
        ring_event(3)
        for copy in list(cross_sends.values()) + list(stat_sends.values()):
            copy.wait_send()

    @pl.when(chip == 1)
    def _():
        wait_swapped()
        for p in range(pairs):
            for i in range(2):
                first = i * tokens
                parts = block(
                    p, qg[first:first + tokens, pair_columns(p)], first + tokens, True,
                    chip_rows + first, chip_rows)
                local_f32[first:first + tokens, pair_columns(p)] = by_head([part[0] for part in parts])
                local_stats[p, first:first + tokens, :] = stats_of(parts)
        ring_event(0)
        ring_event(1)
        for p in range(pairs):
            if p == 1:
                ring_event(2)
            if p == pairs - 1:
                ring_event(3)
            for i in range(2):
                first = i * tokens
                cross_sends[p, i].wait_recv()
                stat_sends[p, i].wait_recv()
                far_stats = jnp.transpose(srx[p, i])
                near_stats = local_stats[p, first:first + tokens, :]
                near, far, total = [], [], []
                for j in range(per_pair):
                    near_top, far_top = near_stats[:, j:j + 1], far_stats[:, j:j + 1]
                    top = jnp.maximum(near_top, far_top)
                    near_factor = jnp.exp2(near_top - top)
                    far_factor = jnp.exp2(far_top - top) * far_stats[:, per_pair + j:per_pair + j + 1]
                    total = near_factor * near_stats[:, per_pair + j:per_pair + j + 1] + far_factor
                    near.append(near_factor / total)
                    far.append(far_factor / total)
                merged = (
                    local_f32[first:first + tokens, pair_columns(p)] * by_head(near)
                    + orx[first:first + tokens, pair_columns(p)].astype(jnp.float32) * by_head(far)
                )
                done_out[first:first + tokens, pair_columns(p)] = merged.astype(jnp.bfloat16)
        final_copy.start()
        final_local.start()
        for copy in query_sends.values():
            copy.wait_send()

    def project(owner):
        product = jnp.zeros((columns, tokens), jnp.float32)
        for n in range(4):
            product += lax.dot_general(
                wg[owner, n], attended[:, n * quarter:(n + 1) * quarter], nt,
                preferred_element_type=jnp.float32)
        out[pl.ds(pl.multiple_of(owner * columns, 8), columns), :] = product.astype(jnp.bfloat16)

    def project_step(step):
        for side in range(2):
            for piece in range(2):
                if step < steps - 1 or piece == side:
                    swap_weight[side, step, piece].wait()
        for side in range(2 if step < steps - 1 else 1):
            project(came_from[side, step])

    ring_event(4)
    for copy in own_copies:
        copy.wait()
    final_local.wait()
    final_copy.wait()
    project(mine)
    project_step(0)
    ring_event(5)
    project_step(1)
    for n in range(6, len(events) + 1):
        ring_event(n)
    for step in range(2, steps):
        project_step(step)

    for copy in gate_copies + swap_copies + list(ring.values()):
        copy.wait_send()


def fused(dp, depth, q, k, v, gate, w):
    tokens, width = q.shape
    columns = w.shape[1]
    half = width // 2
    pairs = half // LANES
    steps = dp // 2
    any_spec = pl.BlockSpec(memory_space=pl.ANY)
    vmem_spec = pl.BlockSpec(memory_space=pltpu.VMEM)
    dma = pltpu.SemaphoreType.DMA
    held = pltpu.VMEM((2 * tokens, half), jnp.bfloat16)
    stats = pltpu.VMEM((pairs, 2, 8, tokens), jnp.float32)
    return pl.pallas_call(
        functools.partial(fused_kernel, dp, depth),
        out_shape=jax.ShapeDtypeStruct((columns * dp, tokens), jnp.bfloat16),
        in_specs=[any_spec, any_spec, any_spec, vmem_spec, any_spec],
        out_specs=vmem_spec,
        scratch_shapes=[
            held, held, held, held,
            pltpu.VMEM((2 * tokens, half), jnp.float32),
            pltpu.VMEM((pairs, 2 * tokens, LANES), jnp.float32),
            held, held, stats, stats, held,
            pltpu.VMEM((tokens, width), jnp.bfloat16),
            pltpu.VMEM((4,) + gate.shape, jnp.float32),
            pltpu.VMEM((dp, 4, columns, width // 4), jnp.bfloat16),
            dma((3,)), dma((3,)), dma((3,)), dma((3,)), dma((3,)),
            dma((pairs, 2)), dma((pairs, 2)),
            dma((pairs, 2)), dma((pairs, 2)), dma((pairs, 2)), dma((pairs, 2)),
            dma((1,)), dma((1,)), dma((1,)),
            dma((2, steps, 2)), dma((2, steps, 2)),
            dma((2, steps, 2)), dma((2, steps, 2)), dma((4,)),
        ],
        compiler_params=pltpu.CompilerParams(
            collective_id=0, has_side_effects=True, vmem_limit_bytes=60 * 1024 * 1024),
    )(q, k, v, gate, w.T).T


def fits(sp, dp, tokens, width, depth, columns):
    return (
        sp == 4 and dp % 2 == 0 and 8 <= dp <= 16
        and width % (4 * LANES) == 0 and width <= 1024 and LANES % depth == 0
        and tokens <= 256 and tokens % LANES == 0
        and (width // depth // sp) % (LANES // depth) == 0
        and LANES // depth <= 4
        and columns % 8 == 0 and columns * dp <= 4096
    )


def attend(query_all, key_all, value_all, gate_all):
    length, width = query_all.shape
    heads = gate_all.shape[0]
    depth = width // heads
    block_rows = min(512, length)
    block_count = length // block_rows
    score_scale = depth ** (-0.5)
    query_blocks = query_all.reshape(block_count, block_rows, heads, depth)
    key_blocks = key_all.reshape(block_count, block_rows, heads, depth)
    value_blocks = value_all.reshape(block_count, block_rows, heads, depth)
    gate_blocks = gate_all.reshape(heads, block_count, block_rows).transpose(1, 0, 2)
    offsets = jnp.arange(block_rows, dtype=jnp.int32)

    def one_block(block_index):
        query_part = lax.dynamic_index_in_dim(query_blocks, block_index, 0, keepdims=False)
        gate_part = lax.dynamic_index_in_dim(gate_blocks, block_index, 0, keepdims=False)
        query_rows = block_index * block_rows + offsets

        def key_step(key_block, carry):
            running_max, running_sum, weighted = carry
            key_part = lax.dynamic_index_in_dim(key_blocks, key_block, 0, keepdims=False)
            value_part = lax.dynamic_index_in_dim(value_blocks, key_block, 0, keepdims=False)
            gate_keys = lax.dynamic_index_in_dim(gate_blocks, key_block, 0, keepdims=False)
            logits = (
                jnp.einsum("qhe,khe->hqk", query_part, key_part, preferred_element_type=jnp.float32)
                * score_scale
            )
            logits = logits + gate_part[:, :, None] - gate_keys[:, None, :]
            key_rows = key_block * block_rows + offsets
            allowed = key_rows[None, :] <= query_rows[:, None]
            logits = jnp.where(allowed[None], logits, -jnp.inf)
            new_max = jnp.maximum(running_max, jnp.max(logits, axis=-1))
            scores = jnp.exp(logits - new_max[..., None])
            factor = jnp.exp(running_max - new_max)
            running_sum = running_sum * factor + jnp.sum(scores, axis=-1)
            weighted = weighted * factor[..., None] + jnp.einsum(
                "hqk,khe->hqe",
                scores.astype(jnp.bfloat16),
                value_part,
                preferred_element_type=jnp.float32,
            )
            return (new_max, running_sum, weighted)

        start_state = (
            jnp.full((heads, block_rows), -jnp.inf, jnp.float32),
            jnp.zeros((heads, block_rows), jnp.float32),
            jnp.zeros((heads, block_rows, depth), jnp.float32),
        )
        final_max, final_sum, weighted = lax.fori_loop(0, block_index + 1, key_step, start_state)
        result = weighted / final_sum[..., None]
        return result.transpose(1, 0, 2).astype(jnp.bfloat16)

    outputs = lax.map(one_block, jnp.arange(block_count, dtype=jnp.int32))
    return outputs.reshape(length, width)


def body(queries, keys, values, cum_gate, out_weight):
    sp, dp = lax.axis_size("sp"), lax.axis_size("dp")
    tokens, width = queries.shape[1:]
    depth = width // (cum_gate.shape[1] * sp)
    if fits(sp, dp, tokens, width, depth, out_weight.shape[1]):
        mixed = fused(dp, depth, queries[0], keys[0], values[0], cum_gate[0], out_weight)
        return mixed[None]
    query_heads, key_heads, value_heads = (
        lax.all_to_all(queries, "sp", split_axis=2, concat_axis=1, tiled=True),
        lax.all_to_all(keys, "sp", split_axis=2, concat_axis=1, tiled=True),
        lax.all_to_all(values, "sp", split_axis=2, concat_axis=1, tiled=True),
    )
    local_out = attend(query_heads[0], key_heads[0], value_heads[0], cum_gate[0])
    attended = lax.all_to_all(local_out[None], "sp", split_axis=1, concat_axis=2, tiled=True)[0]
    group_rows = attended.shape[1] // lax.axis_size("sp")
    own_rows = lax.dynamic_slice_in_dim(
        out_weight, lax.axis_index("sp") * group_rows, group_rows, 0
    )
    full_rows = lax.all_gather(own_rows, "dp", axis=1, tiled=True)
    whole_weight = lax.all_gather(full_rows, "sp", axis=0, tiled=True)
    mixed = jnp.dot(attended, whole_weight, preferred_element_type=jnp.float32)
    return mixed.astype(jnp.bfloat16)[None]


def solution(mesh):
    in_specs = (
        P("dp", "sp", None),
        P("dp", "sp", None),
        P("dp", "sp", None),
        P("dp", "sp", None),
        P(None, "dp"),
    )
    out_specs = P("dp", "sp", None)
    return jax.shard_map(body, mesh=mesh, in_specs=in_specs, out_specs=out_specs, check_vma=False)
```
